32 devices in a mesh: fs: 8 (over z, y), tp: 4 (over x, core).
Axes of the slice: x: 2, y: 2, z: 4, core: 2. Of those that a mesh axis runs over, the one named last changes fastest.
Arguments:
- cotangent: bfloat16 [5120, 1024], P('fs', 'tp'), may hold values from -6 to 6
- inputs: bfloat16 [5120, 1024], P('fs', 'tp'), may hold values from -6 to 6
- pre_act: bfloat16 [5120, 2112], P('fs'), may hold values from -6 to 6
- w_up: bfloat16 [2112, 1024], P('fs', 'tp'), may hold values from -0.1875 to 0.1875
- w_down: bfloat16 [2112, 1024], P('fs', 'tp'), may hold values from -0.125 to 0.125
Outputs:
- grad_input: bfloat16 [5120, 1024], P('fs', 'tp')
- grad_up: float32 [2112, 1024], P('fs', 'tp')
The draws below stay inside these ranges and needn't reach their ends.
All inputs are finite; a program needn't handle non-finite values.
Results may differ from the reference program's by a relative error of at most 0.0049.
Values may be sent and summed in bfloat16 or wider, within the bound.
A program may use at most 64 MiB of HBM per device.

```python
import jax
import jax.numpy as jnp
from jax import lax

D = 1024
FF = 2112
TOKENS = 5120


def strengthened(drawn, stream_key, source, target, shards_of, factor):
    owner, partner = [(jnp.arange(drawn.shape[position]) // (drawn.shape[position] // shards_of)).reshape([-1 if axis == position else 1 for axis in range(drawn.ndim)]) for position in (source, target)]
    chosen = jax.random.permutation(stream_key, shards_of)[partner]
    strong = (owner == chosen) | (owner == (partner + shards_of // 2) % shards_of)
    return jnp.where(strong, factor * drawn, drawn)


def block_levels(stream_key, shape, pieces, low, largest):
    gain, own = 1.0, jax.random.fold_in(stream_key, 6)
    for dim, parts in pieces:
        draws = jnp.exp(jax.random.uniform(jax.random.fold_in(own, dim), (parts,), jnp.float32, low / len(pieces), largest / len(pieces)))
        gain = gain * jnp.repeat(draws, shape[dim] // parts).reshape([-1 if axis == dim else 1 for axis in range(len(shape))])
    return gain


def bell_draw(key, extent, scale, limit, pieces=(), kind=jnp.bfloat16):
    level = block_levels(key, extent, pieces, -0.22, 0.18) if pieces else 1.0
    result = jax.random.normal(key, extent, jnp.float32) * scale * level
    return jnp.minimum(jnp.maximum(result, -limit), limit).astype(kind)


def gaussian_with(key, shape, deviation, reach, pieces, heavy, kind=jnp.bfloat16):
    drawn = deviation * jax.random.normal(key, shape, jnp.float32)
    if pieces:
        drawn = drawn * block_levels(key, shape, pieces, -0.22, 0.18)
    return jnp.clip(strengthened(drawn, jax.random.fold_in(key, 3), *heavy), -reach, reach).astype(kind)


def setup_inputs(seed: int = 0) -> dict:
    key_of = jax.random.split(jax.random.key(seed), 6)
    return {
        "cotangent": bell_draw(key_of[0], (TOKENS, D), 1.0, 6.0, ((0, 8), (1, 4))),
        "inputs": bell_draw(key_of[1], (TOKENS, D), 1.0, 6.0, ((0, 8), (1, 4))),
        "pre_act": gaussian_with(key_of[2], (TOKENS, FF), 1.0, 6.0, ((0, 8),), (0, 1, 8, 2.0)),
        "w_up": bell_draw(key_of[3], (FF, D), D ** -0.5, 0.1875, ((0, 8), (1, 4))),
        "w_down": bell_draw(key_of[4], (FF, D), FF ** -0.5, 0.125, ((0, 8), (1, 4))),
    }


def reference(cotangent, inputs, pre_act, w_up, w_down):
    grad_hidden = lax.dot_general(cotangent, w_down, (((1,), (1,)), ((), ())), preferred_element_type=jnp.float32)
    grad_pre = (2.0 * grad_hidden * jnp.maximum(pre_act.astype(jnp.float32), 0.0)).astype(jnp.bfloat16)
    grad_input = jnp.dot(grad_pre, w_up, preferred_element_type=jnp.float32).astype(jnp.bfloat16)
    summed = lax.dot_general(grad_pre, inputs, (((0,), (0,)), ((), ())), preferred_element_type=jnp.float32)
    grad_up = summed / jnp.sqrt(jnp.float32(TOKENS))
    return (grad_input, grad_up)
```

```python
import functools

import jax
import jax.numpy as jnp
from jax import lax
from jax.experimental import pallas as pl
from jax.experimental.pallas import tpu as pltpu
from jax.sharding import PartitionSpec as P

MESH = pl.DeviceIdType.MESH


def times_rows(left, piece):
    return lax.dot_general(
        left, piece, (((1,), (1,)), ((), ())), preferred_element_type=jnp.float32
    )


def toggled(index, mask, bits):
    for bit in range(bits):
        unit = 2**bit
        index = index + unit * ((mask // unit) % 2) * (1 - 2 * ((index // unit) % 2))
    return index


def kernel(
    n, token_total,
    cot_ref, in_ref, pre_ref, up_ref, down_ref,
    gi_ref, gu_ref,
    cot_buf, down_buf, up_buf, pre_buf, own_part, part_out, part_in,
    local_sem, cot_send, cot_recv, dz_send, dy_send, dx_send, dc_send, dr_send, down_recv,
    uz_send, uy_send, up_recv, part_send, part_recv,
):
    bits = n.bit_length() - 1
    half = n // 2
    f = lax.axis_index("fs")
    t = lax.axis_index("tp")
    width = cot_ref.shape[1]
    rows = down_ref.shape[0]
    t_core = toggled(t, 1, 2)
    t_x = toggled(t, 2, 2)
    t_xcore = toggled(t, 3, 2)

    def seq(i):
        return toggled(f, i, bits)

    def cols(tp):
        return pl.ds(pl.multiple_of(tp * width, width), width)

    def down_slot(src_f, src_t):
        return down_buf.at[src_f, :, cols(src_t)]

    def remote(src, dst, send, recv, fs, tp):
        return pltpu.make_async_remote_copy(
            src_ref=src, dst_ref=dst, send_sem=send, recv_sem=recv,
            device_id=(fs, tp), device_id_type=MESH,
        )

    barrier = pltpu.get_barrier_semaphore()
    peers = [(seq(i), t) for i in range(1, n)] + [(f, t_core), (f, t_x)]
    for peer in peers:
        pl.semaphore_signal(barrier, inc=1, device_id=peer, device_id_type=MESH)
    pl.semaphore_wait(barrier, len(peers))

    def cot_copy(src, src_t, slot, tp):
        return remote(src, cot_buf.at[:, cols(src_t)], cot_send.at[slot], cot_recv.at[src_t], f, tp)

    def down_copy(src, src_f, src_t, send, fs, tp):
        return remote(src, down_slot(src_f, src_t), send, down_recv.at[src_f, src_t], fs, tp)

    def up_copy(src, src_f, send, fs):
        return remote(src, up_buf.at[src_f], send, up_recv.at[src_f], fs, t)

    sent = []

    def go(copy):
        copy.start()
        sent.append(copy)

    go(cot_copy(cot_ref, t, 0, t_core))
    go(cot_copy(cot_ref, t, 1, t_x))
    for k in range(1, half):
        go(down_copy(down_ref, f, t, dz_send.at[k], seq(2 * k), t))
    go(down_copy(down_ref, f, t, dy_send.at[0], seq(1), t))
    go(down_copy(down_ref, f, t, dx_send.at[0], f, t_x))
    go(down_copy(down_ref, f, t, dc_send.at[0], f, t_core))
    for k in range(1, half):
        go(up_copy(up_ref, f, uz_send.at[k], seq(2 * k)))
    go(up_copy(up_ref, f, uy_send.at[0], seq(1)))

    local = [
        pltpu.make_async_copy(cot_ref, cot_buf.at[:, cols(t)], local_sem.at[0]),
        pltpu.make_async_copy(down_ref, down_slot(f, t), local_sem.at[1]),
        pltpu.make_async_copy(up_ref, up_buf.at[f], local_sem.at[2]),
    ]
    for copy in local:
        copy.start()

    for block in range(n):
        pre_buf[block] = pre_ref[:, block * rows : (block + 1) * rows]

    def arrived_down(src_f, src_t):
        down_copy(down_slot(src_f, src_t), src_f, src_t, dz_send.at[0], f, t_core).wait_recv()

    def arrived_up(src_f):
        up_copy(up_buf.at[src_f], src_f, uz_send.at[0], seq(1)).wait_recv()

    def arrived_cot(src_t):
        cot_copy(cot_buf.at[:, cols(src_t)], src_t, 0, t_core).wait_recv()

    def take_own(i):
        src = seq(i)
        arrived_down(src, t)
        block = down_slot(src, t)
        down_copy(block, src, t, dx_send.at[i], f, t_x).start()
        down_copy(block, src, t, dc_send.at[i], f, t_core).start()

        @pl.when(i % 2 == 0)
        def _():
            down_copy(block, src, t, dy_send.at[i // 2], seq(1), t).start()

    for copy in local:
        copy.wait()
    take_own(1)
    arrived_cot(t_x)
    go(cot_copy(cot_buf.at[:, cols(t_x)], t_x, 2, t_core))
    arrived_cot(t_core)
    arrived_cot(t_xcore)

    def step(i, carry):
        @pl.when(i < n - 2)
        def _():
            take_own(i + 2)

        @pl.when(i < n)
        def _():
            src = seq(i)
            arrived_down(src, t_x)
            down_copy(down_slot(src, t_x), src, t_x, dr_send.at[i], f, t_core).start()

            @pl.when((i % 2 == 0) & (i > 0))
            def _():
                arrived_up(src)
                up_copy(up_buf.at[src], src, uy_send.at[i // 2], seq(1)).start()

        @pl.when(i > 0)
        def _():
            j = i - 1
            src = seq(j)
            arrived_down(src, t_core)
            arrived_down(src, t_xcore)
            hidden = times_rows(cot_buf[...], down_buf[src])
            grad_pre = (
                2.0 * hidden * jnp.maximum(pre_buf[src].astype(jnp.float32), 0.0)
            ).astype(jnp.bfloat16)
            pre_buf[src] = grad_pre
            part = lax.dot_general(
                grad_pre, in_ref[...], (((0,), (0,)), ((), ())), preferred_element_type=jnp.float32
            )

            @pl.when(j == 0)
            def _():
                own_part[...] = part

            @pl.when(j > 0)
            def _():
                part_out[j] = part.astype(jnp.bfloat16)
                remote(part_out.at[j], part_in.at[f], part_send.at[j], part_recv.at[f], src, t).start()

        return carry

    lax.fori_loop(0, n + 1, step, 0)

    for i in range(1, n, 2):
        arrived_up(seq(i))
    gi = jnp.zeros(gi_ref.shape, jnp.float32)
    for block in range(n):
        gi = gi + jnp.dot(pre_buf[block], up_buf[block], preferred_element_type=jnp.float32)
    gi_ref[...] = gi.astype(gi_ref.dtype)

    total = own_part[...]
    for i in range(1, n):
        src = seq(i)
        remote(part_out.at[i], part_in.at[src], part_send.at[i], part_recv.at[src], src, t).wait_recv()
        total = total + part_in[src].astype(jnp.float32)
    gu_ref[...] = total / jnp.sqrt(jnp.float32(token_total))

    for copy in sent:
        copy.wait_send()
    for i in range(1, n):
        src = seq(i)
        block = down_slot(src, t)
        down_copy(block, src, t, dx_send.at[i], f, t_x).wait_send()
        down_copy(block, src, t, dc_send.at[i], f, t_core).wait_send()
        remote(part_out.at[i], part_in.at[f], part_send.at[i], part_recv.at[f], src, t).wait_send()
        if i % 2 == 0:
            down_copy(block, src, t, dy_send.at[i // 2], seq(1), t).wait_send()
            up_copy(up_buf.at[src], src, uy_send.at[i // 2], seq(1)).wait_send()
    for i in range(n):
        src = seq(i)
        down_copy(down_slot(src, t_x), src, t_x, dr_send.at[i], f, t_core).wait_send()


def fused(n, tp, cotangent, inputs, pre_act, w_up, w_down):
    tokens, width = cotangent.shape
    rows = w_down.shape[0]
    dma = pltpu.SemaphoreType.DMA
    half = n // 2
    return pl.pallas_call(
        functools.partial(kernel, n, tokens * n),
        out_shape=(
            jax.ShapeDtypeStruct((tokens, width), jnp.bfloat16),
            jax.ShapeDtypeStruct((rows, width), jnp.float32),
        ),
        in_specs=[pl.BlockSpec(memory_space=pltpu.VMEM)] * 5,
        out_specs=(pl.BlockSpec(memory_space=pltpu.VMEM),) * 2,
        scratch_shapes=[
            pltpu.VMEM((tokens, tp * width), jnp.bfloat16),
            pltpu.VMEM((n, rows, tp * width), jnp.bfloat16),
            pltpu.VMEM((n, rows, width), jnp.bfloat16),
            pltpu.VMEM((n, tokens, rows), jnp.bfloat16),
            pltpu.VMEM((rows, width), jnp.float32),
            pltpu.VMEM((n, rows, width), jnp.bfloat16),
            pltpu.VMEM((n, rows, width), jnp.bfloat16),
            dma((3,)),
            dma((3,)), dma((tp,)),
            dma((half,)), dma((half,)), dma((n,)), dma((n,)), dma((n,)), dma((n, tp)),
            dma((half,)), dma((half,)), dma((n,)),
            dma((n,)), dma((n,)),
        ],
        compiler_params=pltpu.CompilerParams(
            collective_id=0, has_side_effects=True, vmem_limit_bytes=60 * 2**20
        ),
    )(cotangent, inputs, pre_act, w_up, w_down)


def gathered(cotangent, inputs, pre_act, w_up, w_down):
    token_total = cotangent.shape[0] * lax.axis_size("fs")
    full_cotangent = lax.all_gather(cotangent, "tp", axis=1, tiled=True)
    down_whole = lax.all_gather(w_down, "tp", axis=1, tiled=True)
    grad_hidden = times_rows(full_cotangent, lax.all_gather(down_whole, "fs", axis=0, tiled=True))
    grad_pre = (2.0 * grad_hidden * jnp.maximum(pre_act.astype(jnp.float32), 0.0)).astype(
        jnp.bfloat16
    )
    grad_input = jnp.dot(
        grad_pre, lax.all_gather(w_up, "fs", axis=0, tiled=True), preferred_element_type=jnp.float32
    )
    grad_share = lax.psum_scatter(
        lax.dot_general(
            grad_pre, inputs, (((0,), (0,)), ((), ())), preferred_element_type=jnp.float32
        ),
        "fs",
        scatter_dimension=0,
        tiled=True,
    )
    grad_up = grad_share / jnp.sqrt(jnp.float32(token_total))
    return (grad_input.astype(jnp.bfloat16), grad_up)


def solution(mesh):
    n, tp = mesh.shape["fs"], mesh.shape["tp"]

    def local(cotangent, inputs, pre_act, w_up, w_down):
        rows, width = w_down.shape
        fits = tp == 4 and 4 <= n <= 16 and n & (n - 1) == 0 and rows % 8 == 0 and width % 128 == 0
        if fits:
            return fused(n, tp, cotangent, inputs, pre_act, w_up, w_down)
        return gathered(cotangent, inputs, pre_act, w_up, w_down)

    return jax.shard_map(
        local,
        mesh=mesh,
        in_specs=(P("fs", "tp"), P("fs", "tp"), P("fs", None), P("fs", "tp"), P("fs", "tp")),
        out_specs=(P("fs", "tp"), P("fs", "tp")),
        check_vma=False,
    )
```

```python
import functools

import jax
import jax.numpy as jnp
from jax import lax
from jax.experimental import pallas as pl
from jax.experimental.pallas import tpu as pltpu
from jax.sharding import PartitionSpec as P

MESH = pl.DeviceIdType.MESH


def times_rows(left, piece):
    return lax.dot_general(
        left, piece, (((1,), (1,)), ((), ())), preferred_element_type=jnp.float32
    )


def toggled(index, mask, bits):
    for bit in range(bits):
        unit = 2**bit
        index = index + unit * ((mask // unit) % 2) * (1 - 2 * ((index // unit) % 2))
    return index


def kernel(
    n, token_total,
    cot_ref, in_ref, pre_ref, up_ref, down_ref,
    gi_ref, gu_ref,
    cot_buf, cot_turned, down_buf, up_buf, pre_buf, held, y_out, y_in, z_out, z_in,
    local_sem, cot_send, cot_recv, dz_send, dy_send, dx_send, dc_send, dr_send, down_recv,
    uz_send, uy_send, up_recv, ys_send, ys_recv, zs_send, zs_recv,
):
    bits = n.bit_length() - 1
    half = n // 2
    f = lax.axis_index("fs")
    t = lax.axis_index("tp")
    width = cot_ref.shape[1]
    t_core = toggled(t, 1, 2)
    t_x = toggled(t, 2, 2)
    t_xcore = toggled(t, 3, 2)
    f_y = toggled(f, 1, 1)

    def split(i):
        pair = i // 2
        last = pair // (half - 1)
        return (pair + 1) % half, i % 2 + last * (1 - 2 * (i % 2))

    def seq(i):
        far, across = split(i)
        return toggled(f, 2 * far + across, bits)

    def cols(tp):
        return pl.ds(pl.multiple_of(tp * width, width), width)

    def down_slot(src_f, src_t):
        return down_buf.at[src_f, :, cols(src_t)]

    def remote(src, dst, send, recv, fs, tp):
        return pltpu.make_async_remote_copy(
            src_ref=src, dst_ref=dst, send_sem=send, recv_sem=recv,
            device_id=(fs, tp), device_id_type=MESH,
        )

    def cot_copy(src, src_t, slot, tp):
        return remote(src, cot_buf.at[:, cols(src_t)], cot_send.at[slot], cot_recv.at[src_t], f, tp)

    def down_copy(src, src_f, src_t, send, fs, tp):
        return remote(src, down_slot(src_f, src_t), send, down_recv.at[src_f, src_t], fs, tp)

    def up_copy(src, src_f, send, fs):
        return remote(src, up_buf.at[src_f], send, up_recv.at[src_f], fs, t)

    def y_copy(pair):
        return remote(y_out.at[pair], y_in.at[pair], ys_send.at[pair], ys_recv.at[pair], f_y, t)

    def z_copy(pair):
        owner = toggled(f, 2 * (pair + 1), bits)
        return remote(z_out.at[pair], z_in.at[pair], zs_send.at[pair], zs_recv.at[pair], owner, t)

    local = [
        pltpu.make_async_copy(cot_ref, cot_buf.at[:, cols(t)], local_sem.at[0]),
        pltpu.make_async_copy(down_ref, down_slot(f, t), local_sem.at[1]),
        pltpu.make_async_copy(up_ref, up_buf.at[f], local_sem.at[2]),
        pltpu.make_async_copy(pre_ref, pre_buf, local_sem.at[3]),
    ]
    for copy in local:
        copy.start()

    barrier = pltpu.get_barrier_semaphore()
    far_peers = [toggled(f, 2 * k, bits) for k in range(1, half)]
    peers = [(peer, t) for peer in far_peers] + [(f_y, t), (f, t_core), (f, t_x)]
    for peer in peers:
        pl.semaphore_signal(barrier, inc=1, device_id=peer, device_id_type=MESH)
    pl.semaphore_wait(barrier, len(peers))

    sent = []

    def go(copy):
        copy.start()
        sent.append(copy)

    go(cot_copy(cot_ref, t, 1, t_x))
    for k in range(1, half):
        go(down_copy(down_ref, f, t, dz_send.at[k], far_peers[k - 1], t))
    go(down_copy(down_ref, f, t, dy_send.at[0], f_y, t))
    go(cot_copy(cot_ref, t, 0, t_core))
    for k in range(1, half):
        go(up_copy(up_ref, f, uz_send.at[k], far_peers[k - 1]))

    def arrived_down(src_f, src_t):
        down_copy(down_slot(src_f, src_t), src_f, src_t, dz_send.at[0], f, t_core).wait_recv()

    def arrived_up(src_f):
        up_copy(up_buf.at[src_f], src_f, uz_send.at[0], f_y).wait_recv()

    def arrived_cot(src_t):
        cot_copy(cot_buf.at[:, cols(src_t)], src_t, 0, t_core).wait_recv()

    def take_own(i):
        far, across = split(i)
        src = seq(i)

        @pl.when(far + across > 0)
        def _():
            arrived_down(src, t)

        block = down_slot(src, t)
        down_copy(block, src, t, dx_send.at[i], f, t_x).start()
        down_copy(block, src, t, dc_send.at[i], f, t_core).start()

        @pl.when((far > 0) & (across == 0))
        def _():
            down_copy(block, src, t, dy_send.at[far], f_y, t).start()

    local[1].wait()
    take_own(0)
    arrived_cot(t_x)
    go(cot_copy(cot_buf.at[:, cols(t_x)], t_x, 2, t_core))
    take_own(1)
    go(up_copy(up_ref, f, uy_send.at[0], f_y))
    local[0].wait()
    arrived_cot(t_core)
    arrived_cot(t_xcore)
    cot_turned[...] = cot_buf[...].T
    local[2].wait()
    local[3].wait()

    def step(i, carry):
        @pl.when(i < n - 2)
        def _():
            take_own(i + 2)

        @pl.when(i < n)
        def _():
            src = seq(i)
            arrived_down(src, t_x)
            down_copy(down_slot(src, t_x), src, t_x, dr_send.at[i], f, t_core).start()

        @pl.when((i >= 3) & (i < half + 2))
        def _():
            k = i - 2
            src = toggled(f, 2 * k, bits)
            arrived_up(src)
            up_copy(up_buf.at[src], src, uy_send.at[k], f_y).start()

        @pl.when((i >= 4) & (i % 2 == 0))
        def _():
            pair = i // 2 - 2
            y_copy(pair).wait_recv()
            z_out[pair] = (held[pair] + y_in[pair].astype(jnp.float32)).astype(jnp.bfloat16)
            z_copy(pair).start()

        @pl.when(i > 0)
        def _():
            j = i - 1
            src = seq(j)
            pair = j // 2
            arrived_down(src, t_core)
            arrived_down(src, t_xcore)
            hidden = jnp.dot(down_buf[src], cot_turned[...], preferred_element_type=jnp.float32)
            grad_pre = (
                2.0 * hidden * jnp.maximum(pre_buf[src].astype(jnp.float32), 0.0)
            ).astype(jnp.bfloat16)
            pre_buf[src] = grad_pre
            part = jnp.dot(grad_pre, in_ref[...], preferred_element_type=jnp.float32)
            _, across = split(j)

            @pl.when(across == 0)
            def _():
                held[pair] = part

            @pl.when(across == 1)
            def _():
                y_out[pair] = part.astype(jnp.bfloat16)
                y_copy(pair).start()

        return carry

    lax.fori_loop(0, n + 1, step, 0)

    for k in range(half):
        arrived_up(toggled(f, 2 * k + 1, bits))
    gi = jnp.zeros(gi_ref.shape, jnp.float32)
    for block in range(n):
        gi = gi + lax.dot_general(
            pre_buf[block], up_buf[block], (((0,), (0,)), ((), ())),
            preferred_element_type=jnp.float32,
        )
    gi_ref[...] = gi.astype(gi_ref.dtype)

    total = held[half - 1]
    for pair in range(half - 1):
        z_copy(pair).wait_recv()
        total = total + z_in[pair].astype(jnp.float32)
    y_copy(half - 1).wait_recv()
    total = total + y_in[half - 1].astype(jnp.float32)
    gu_ref[...] = total / jnp.sqrt(jnp.float32(token_total))

    for copy in sent:
        copy.wait_send()
    for i in range(n):
        src = seq(i)
        far, across = split(i)
        block = down_slot(src, t)
        down_copy(block, src, t, dx_send.at[i], f, t_x).wait_send()
        down_copy(block, src, t, dc_send.at[i], f, t_core).wait_send()
        down_copy(down_slot(src, t_x), src, t_x, dr_send.at[i], f, t_core).wait_send()
        if far > 0 and across == 0:
            down_copy(block, src, t, dy_send.at[far], f_y, t).wait_send()
            up_copy(up_buf.at[src], src, uy_send.at[far], f_y).wait_send()
    for pair in range(half):
        y_copy(pair).wait_send()
        if pair < half - 1:
            z_copy(pair).wait_send()


def fused(n, tp, cotangent, inputs, pre_act, w_up, w_down):
    tokens, width = cotangent.shape
    rows = w_down.shape[0]
    dma = pltpu.SemaphoreType.DMA
    half = n // 2
    vmem = pl.BlockSpec(memory_space=pltpu.VMEM)
    return pl.pallas_call(
        functools.partial(kernel, n, tokens * n),
        out_shape=(
            jax.ShapeDtypeStruct((tokens, width), jnp.bfloat16),
            jax.ShapeDtypeStruct((rows, width), jnp.float32),
        ),
        in_specs=[vmem, vmem, pl.BlockSpec(memory_space=pl.ANY), vmem, vmem],
        out_specs=(vmem, vmem),
        scratch_shapes=[
            pltpu.VMEM((tokens, tp * width), jnp.bfloat16),
            pltpu.VMEM((tp * width, tokens), jnp.bfloat16),
            pltpu.VMEM((n, rows, tp * width), jnp.bfloat16),
            pltpu.VMEM((n, rows, width), jnp.bfloat16),
            pltpu.VMEM((n, rows, tokens), jnp.bfloat16),
            pltpu.VMEM((half, rows, width), jnp.float32),
            pltpu.VMEM((half, rows, width), jnp.bfloat16),
            pltpu.VMEM((half, rows, width), jnp.bfloat16),
            pltpu.VMEM((half - 1, rows, width), jnp.bfloat16),
            pltpu.VMEM((half - 1, rows, width), jnp.bfloat16),
            dma((4,)),
            dma((3,)), dma((tp,)),
            dma((half,)), dma((half,)), dma((n,)), dma((n,)), dma((n,)), dma((n, tp)),
            dma((half,)), dma((half,)), dma((n,)),
            dma((half,)), dma((half,)), dma((half - 1,)), dma((half - 1,)),
        ],
        compiler_params=pltpu.CompilerParams(
            collective_id=0, has_side_effects=True, vmem_limit_bytes=60 * 2**20
        ),
    )(cotangent, inputs, pre_act.T.reshape(n, rows, tokens), w_up, w_down)


def gathered(cotangent, inputs, pre_act, w_up, w_down):
    token_total = cotangent.shape[0] * lax.axis_size("fs")
    full_cotangent = lax.all_gather(cotangent, "tp", axis=1, tiled=True)
    down_whole = lax.all_gather(w_down, "tp", axis=1, tiled=True)
    grad_hidden = times_rows(full_cotangent, lax.all_gather(down_whole, "fs", axis=0, tiled=True))
    grad_pre = (2.0 * grad_hidden * jnp.maximum(pre_act.astype(jnp.float32), 0.0)).astype(
        jnp.bfloat16
    )
    grad_input = jnp.dot(
        grad_pre, lax.all_gather(w_up, "fs", axis=0, tiled=True), preferred_element_type=jnp.float32
    )
    grad_share = lax.psum_scatter(
        lax.dot_general(
            grad_pre, inputs, (((0,), (0,)), ((), ())), preferred_element_type=jnp.float32
        ),
        "fs",
        scatter_dimension=0,
        tiled=True,
    )
    grad_up = grad_share / jnp.sqrt(jnp.float32(token_total))
    return (grad_input.astype(jnp.bfloat16), grad_up)


def solution(mesh):
    n, tp = mesh.shape["fs"], mesh.shape["tp"]

    def local(cotangent, inputs, pre_act, w_up, w_down):
        rows, width = w_down.shape
        fits = tp == 4 and 4 <= n <= 16 and n & (n - 1) == 0 and rows % 8 == 0 and width % 128 == 0
        if fits:
            return fused(n, tp, cotangent, inputs, pre_act, w_up, w_down)
        return gathered(cotangent, inputs, pre_act, w_up, w_down)

    return jax.shard_map(
        local,
        mesh=mesh,
        in_specs=(P("fs", "tp"), P("fs", "tp"), P("fs", None), P("fs", "tp"), P("fs", "tp")),
        out_specs=(P("fs", "tp"), P("fs", "tp")),
        check_vma=False,
    )
```

```python
import functools

import jax
import jax.numpy as jnp
from jax import lax
from jax.experimental import pallas as pl
from jax.experimental.pallas import tpu as pltpu
from jax.sharding import PartitionSpec as P

MESH = pl.DeviceIdType.MESH


def times_rows(left, piece):
    return lax.dot_general(
        left, piece, (((1,), (1,)), ((), ())), preferred_element_type=jnp.float32
    )


def toggled(index, mask, bits):
    for bit in range(bits):
        unit = 2**bit
        index = index + unit * ((mask // unit) % 2) * (1 - 2 * ((index // unit) % 2))
    return index


def kernel(
    n, token_total,
    cot_ref, in_ref, pre_ref, up_ref, down_ref,
    gi_ref, gu_ref,
    cot_buf, cot_turned, down_buf, up_buf, pre_buf, held, y_out, y_in, z_out, z_in,
    local_sem, cot_send, cot_recv, dz_send, dy_send, dx_send, dc_send, dr_send, down_recv,
    uz_send, uy_send, up_recv, ys_send, ys_recv, zs_send, zs_recv,
):
    bits = n.bit_length() - 1
    half = n // 2
    f = lax.axis_index("fs")
    t = lax.axis_index("tp")
    width = cot_ref.shape[1]
    t_core = toggled(t, 1, 2)
    t_x = toggled(t, 2, 2)
    t_xcore = toggled(t, 3, 2)
    f_y = toggled(f, 1, 1)

    def split(i):
        pair = i // 2
        last = pair // (half - 1)
        return (pair + 1) % half, i % 2 + last * (1 - 2 * (i % 2))

    def seq(i):
        far, across = split(i)
        return toggled(f, 2 * far + across, bits)

    def cols(tp):
        return pl.ds(pl.multiple_of(tp * width, width), width)

    def down_slot(src_f, src_t):
        return down_buf.at[src_f, :, cols(src_t)]

    def remote(src, dst, send, recv, fs, tp):
        return pltpu.make_async_remote_copy(
            src_ref=src, dst_ref=dst, send_sem=send, recv_sem=recv,
            device_id=(fs, tp), device_id_type=MESH,
        )

    def cot_copy(src, src_t, slot, tp):
        return remote(src, cot_buf.at[:, cols(src_t)], cot_send.at[slot], cot_recv.at[src_t], f, tp)

    def down_copy(src, src_f, src_t, send, fs, tp):
        return remote(src, down_slot(src_f, src_t), send, down_recv.at[src_f, src_t], fs, tp)

    def up_copy(src, src_f, send, fs):
        return remote(src, up_buf.at[src_f], send, up_recv.at[src_f], fs, t)

    def y_copy(pair):
        return remote(y_out.at[pair], y_in.at[pair], ys_send.at[pair], ys_recv.at[pair], f_y, t)

    def z_copy(pair):
        owner = toggled(f, 2 * (pair + 1), bits)
        return remote(z_out.at[pair], z_in.at[pair], zs_send.at[pair], zs_recv.at[pair], owner, t)

    local = [
        pltpu.make_async_copy(cot_ref, cot_buf.at[:, cols(t)], local_sem.at[0]),
        pltpu.make_async_copy(down_ref, down_slot(f, t), local_sem.at[1]),
        pltpu.make_async_copy(up_ref, up_buf.at[f], local_sem.at[2]),
        pltpu.make_async_copy(pre_ref, pre_buf, local_sem.at[3]),
    ]
    for copy in local:
        copy.start()

    barrier = pltpu.get_barrier_semaphore()
    far_peers = [toggled(f, 2 * k, bits) for k in range(1, half)]
    peers = [(peer, t) for peer in far_peers] + [(f_y, t), (f, t_core), (f, t_x)]
    for peer in peers:
        pl.semaphore_signal(barrier, inc=1, device_id=peer, device_id_type=MESH)
    pl.semaphore_wait(barrier, len(peers))

    sent = []

    def go(copy):
        copy.start()
        sent.append(copy)

    go(cot_copy(cot_ref, t, 1, t_x))
    for k in range(1, half):
        go(down_copy(down_ref, f, t, dz_send.at[k], far_peers[k - 1], t))
    go(down_copy(down_ref, f, t, dy_send.at[0], f_y, t))
    go(cot_copy(cot_ref, t, 0, t_core))

    def arrived_down(src_f, src_t):
        down_copy(down_slot(src_f, src_t), src_f, src_t, dz_send.at[0], f, t_core).wait_recv()

    def arrived_up(src_f):
        up_copy(up_buf.at[src_f], src_f, uz_send.at[0], f_y).wait_recv()

    def arrived_cot(src_t):
        cot_copy(cot_buf.at[:, cols(src_t)], src_t, 0, t_core).wait_recv()

    def take_own(i):
        far, across = split(i)
        src = seq(i)

        @pl.when(far + across > 0)
        def _():
            arrived_down(src, t)

        block = down_slot(src, t)
        down_copy(block, src, t, dx_send.at[i], f, t_x).start()
        down_copy(block, src, t, dc_send.at[i], f, t_core).start()

        @pl.when((far > 0) & (across == 0))
        def _():
            down_copy(block, src, t, dy_send.at[far], f_y, t).start()

    local[1].wait()
    take_own(0)
    arrived_cot(t_x)
    go(cot_copy(cot_buf.at[:, cols(t_x)], t_x, 2, t_core))
    take_own(1)
    for k in range(1, half):
        go(up_copy(up_ref, f, uz_send.at[k], far_peers[k - 1]))
    go(up_copy(up_ref, f, uy_send.at[0], f_y))
    local[0].wait()
    arrived_cot(t_core)
    arrived_cot(t_xcore)
    cot_turned[...] = cot_buf[...].T
    local[2].wait()
    local[3].wait()

    def step(i, carry):
        @pl.when((i < n - 1) & (i > 0))
        def _():
            take_own(i + 1)

        @pl.when(i < n)
        def _():
            src = seq(i)
            arrived_down(src, t_x)
            down_copy(down_slot(src, t_x), src, t_x, dr_send.at[i], f, t_core).start()

        @pl.when((i >= 3) & (i < half + 2))
        def _():
            k = i - 2
            src = toggled(f, 2 * k, bits)
            arrived_up(src)
            up_copy(up_buf.at[src], src, uy_send.at[k], f_y).start()

        @pl.when(i > 0)
        def _():
            j = i - 1
            src = seq(j)
            pair = j // 2
            arrived_down(src, t_core)
            arrived_down(src, t_xcore)
            hidden = jnp.dot(down_buf[src], cot_turned[...], preferred_element_type=jnp.float32)
            grad_pre = (
                2.0 * hidden * jnp.maximum(pre_buf[src].astype(jnp.float32), 0.0)
            ).astype(jnp.bfloat16)
            pre_buf[src] = grad_pre
            part = jnp.dot(grad_pre, in_ref[...], preferred_element_type=jnp.float32)
            _, across = split(j)

            @pl.when(across == 0)
            def _():
                held[pair] = part

            @pl.when(across == 1)
            def _():
                y_out[pair] = part.astype(jnp.bfloat16)
                y_copy(pair).start()

        @pl.when((i >= 3) & (i % 2 == 1))
        def _():
            pair = (i - 3) // 2
            y_copy(pair).wait_recv()
            z_out[pair] = (held[pair] + y_in[pair].astype(jnp.float32)).astype(jnp.bfloat16)
            z_copy(pair).start()

        return carry

    lax.fori_loop(0, n + 1, step, 0)

    for k in range(half):
        arrived_up(toggled(f, 2 * k + 1, bits))
    gi = jnp.zeros(gi_ref.shape, jnp.float32)
    for block in range(n):
        gi = gi + lax.dot_general(
            pre_buf[block], up_buf[block], (((0,), (0,)), ((), ())),
            preferred_element_type=jnp.float32,
        )
    gi_ref[...] = gi.astype(gi_ref.dtype)

    total = held[half - 1]
    for pair in range(half - 1):
        z_copy(pair).wait_recv()
        total = total + z_in[pair].astype(jnp.float32)
    y_copy(half - 1).wait_recv()
    total = total + y_in[half - 1].astype(jnp.float32)
    gu_ref[...] = total / jnp.sqrt(jnp.float32(token_total))

    for copy in sent:
        copy.wait_send()
    for i in range(n):
        src = seq(i)
        far, across = split(i)
        block = down_slot(src, t)
        down_copy(block, src, t, dx_send.at[i], f, t_x).wait_send()
        down_copy(block, src, t, dc_send.at[i], f, t_core).wait_send()
        down_copy(down_slot(src, t_x), src, t_x, dr_send.at[i], f, t_core).wait_send()
        if far > 0 and across == 0:
            down_copy(block, src, t, dy_send.at[far], f_y, t).wait_send()
            up_copy(up_buf.at[src], src, uy_send.at[far], f_y).wait_send()
    for pair in range(half):
        y_copy(pair).wait_send()
        if pair < half - 1:
            z_copy(pair).wait_send()


def settle(gi_ref, gu_ref, gi_out, gu_out):
    gi_out[...] = gi_ref[...]
    gu_out[...] = gu_ref[...]


def fused(n, tp, cotangent, inputs, pre_act, w_up, w_down):
    tokens, width = cotangent.shape
    rows = w_down.shape[0]
    dma = pltpu.SemaphoreType.DMA
    half = n // 2
    vmem = pl.BlockSpec(memory_space=pltpu.VMEM)
    shapes = (
        jax.ShapeDtypeStruct((tokens, width), jnp.bfloat16),
        jax.ShapeDtypeStruct((rows, width), jnp.float32),
    )
    results = pl.pallas_call(
        functools.partial(kernel, n, tokens * n),
        out_shape=shapes,
        in_specs=[vmem, vmem, pl.BlockSpec(memory_space=pl.ANY), vmem, vmem],
        out_specs=(vmem, vmem),
        scratch_shapes=[
            pltpu.VMEM((tokens, tp * width), jnp.bfloat16),
            pltpu.VMEM((tp * width, tokens), jnp.bfloat16),
            pltpu.VMEM((n, rows, tp * width), jnp.bfloat16),
            pltpu.VMEM((n, rows, width), jnp.bfloat16),
            pltpu.VMEM((n, rows, tokens), jnp.bfloat16),
            pltpu.VMEM((half, rows, width), jnp.float32),
            pltpu.VMEM((half, rows, width), jnp.bfloat16),
            pltpu.VMEM((half, rows, width), jnp.bfloat16),
            pltpu.VMEM((half - 1, rows, width), jnp.bfloat16),
            pltpu.VMEM((half - 1, rows, width), jnp.bfloat16),
            dma((4,)),
            dma((3,)), dma((tp,)),
            dma((half,)), dma((half,)), dma((n,)), dma((n,)), dma((n,)), dma((n, tp)),
            dma((half,)), dma((half,)), dma((n,)),
            dma((half,)), dma((half,)), dma((half - 1,)), dma((half - 1,)),
        ],
        compiler_params=pltpu.CompilerParams(
            collective_id=0, has_side_effects=True, vmem_limit_bytes=60 * 2**20
        ),
    )(cotangent, inputs, pre_act.T.reshape(n, rows, tokens), w_up, w_down)
    return pl.pallas_call(
        settle, out_shape=shapes, in_specs=[vmem, vmem], out_specs=(vmem, vmem)
    )(*results)


def gathered(cotangent, inputs, pre_act, w_up, w_down):
    token_total = cotangent.shape[0] * lax.axis_size("fs")
    full_cotangent = lax.all_gather(cotangent, "tp", axis=1, tiled=True)
    down_whole = lax.all_gather(w_down, "tp", axis=1, tiled=True)
    grad_hidden = times_rows(full_cotangent, lax.all_gather(down_whole, "fs", axis=0, tiled=True))
    grad_pre = (2.0 * grad_hidden * jnp.maximum(pre_act.astype(jnp.float32), 0.0)).astype(
        jnp.bfloat16
    )
    grad_input = jnp.dot(
        grad_pre, lax.all_gather(w_up, "fs", axis=0, tiled=True), preferred_element_type=jnp.float32
    )
    grad_share = lax.psum_scatter(
        lax.dot_general(
            grad_pre, inputs, (((0,), (0,)), ((), ())), preferred_element_type=jnp.float32
        ),
        "fs",
        scatter_dimension=0,
        tiled=True,
    )
    grad_up = grad_share / jnp.sqrt(jnp.float32(token_total))
    return (grad_input.astype(jnp.bfloat16), grad_up)


def solution(mesh):
    n, tp = mesh.shape["fs"], mesh.shape["tp"]

    def local(cotangent, inputs, pre_act, w_up, w_down):
        rows, width = w_down.shape
        fits = tp == 4 and 4 <= n <= 16 and n & (n - 1) == 0 and rows % 8 == 0 and width % 128 == 0
        if fits:
            return fused(n, tp, cotangent, inputs, pre_act, w_up, w_down)
        return gathered(cotangent, inputs, pre_act, w_up, w_down)

    return jax.shard_map(
        local,
        mesh=mesh,
        in_specs=(P("fs", "tp"), P("fs", "tp"), P("fs", None), P("fs", "tp"), P("fs", "tp")),
        out_specs=(P("fs", "tp"), P("fs", "tp")),
        check_vma=False,
    )
```
